32 devices in a mesh: sp: 4 (over z), dp: 8 (over y, x, core).
Axes of the slice: x: 2, y: 2, z: 4, core: 2. Of those that a mesh axis runs over, the one named last changes fastest.
Arguments:
- query_rows: bfloat16 [8, 512, 1024], P('dp', 'sp'), may hold values from -5.5 to 5.5
- key_rows: bfloat16 [8, 512, 1024], P('dp', 'sp'), may hold values from -5.5 to 5.5
- value_rows: bfloat16 [8, 512, 1024], P('dp', 'sp'), may hold values from -6 to 6
- lambdas: float32 [8], replicated, may hold values from 0.3 to 0.8
- query_gain: float32 [64], replicated, may hold values from 1.1 to 8
- key_gain: float32 [64], replicated, may hold values from 1.1 to 8
- sub_gain: float32 [128], replicated, may hold values from 0.1 to 1.9
- out_weight: bfloat16 [1024, 2048], P(None, 'dp'), may hold values from -0.1875 to 0.1875
Outputs:
- attended: bfloat16 [8, 512, 2048], P('dp', 'sp')
The draws below stay inside these ranges and needn't reach their ends.
All inputs are finite; a program needn't handle non-finite values.
Results may differ from the reference program's by a relative error of at most 0.0025.
The reference program's roundings to bfloat16 on the way count: a program that leaves them out, or rounds other values in their place, can miss the bound.
Values may be sent and summed in bfloat16 or wider, within the bound.
A program may use at most 64 MiB of HBM per device.

```python
import jax
import jax.numpy as jnp
from jax import lax

D = 2048
HEADS = 8
HK = 64
HV = 128
LENGTH = 512
SEQS = 8


def key_field(key):
    full_shape = (SEQS, LENGTH, 2 * HEADS * HK)
    key_base = jnp.clip(jax.random.normal(jax.random.fold_in(key, 101), full_shape, jnp.float32), -5.0, 5.0)
    return key_base


def draw_key_rows(key, part):
    return key_field(key).astype(jnp.bfloat16)


def draw_query_rows(key, part):
    full_shape = (SEQS, LENGTH, 2 * HEADS * HK)
    drawn_rows = jnp.clip(jax.random.normal(jax.random.fold_in(key, 107), full_shape, jnp.float32), -5.0, 5.0)
    return drawn_rows.astype(jnp.bfloat16)


def draw_query_gain(key, part):
    uniform_draw = jax.random.uniform(jax.random.fold_in(key, 211), (HK,), jnp.float32)
    return 1.1 + 0.5 * uniform_draw


def draw_key_gain(key, part):
    uniform_draw = jax.random.uniform(jax.random.fold_in(key, 223), (HK,), jnp.float32)
    return 1.1 + 0.5 * uniform_draw


def block_scale(own_key, shape, split, least, top_value):
    gain, own = 1.0, jax.random.fold_in(own_key, 6)
    for dim, shards_of in split:
        steps = jnp.exp(jax.random.uniform(jax.random.fold_in(own, dim), (shards_of,), jnp.float32, least / len(split), top_value / len(split)))
        gain = gain * jnp.repeat(steps, shape[dim] // shards_of).reshape([-1 if axis == dim else 1 for axis in range(len(shape))])
    return gain


def bell_draw(own_key, dims, scale, most, shards=(), kind=jnp.bfloat16):
    array = scale * jax.random.normal(own_key, dims, jnp.float32)
    if shards:
        array = array * block_scale(own_key, dims, shards, -0.22, 0.18)
    return jnp.clip(array, -most, most).astype(kind)


def setup_inputs(seed: int = 0) -> dict:
    keys = jax.random.split(jax.random.key(seed), 9)
    return {
        "query_rows": draw_query_rows(jax.random.fold_in(keys[8], 71), 0),
        "key_rows": draw_key_rows(jax.random.fold_in(keys[8], 71), 0),
        "value_rows": bell_draw(keys[2], (SEQS, LENGTH, HEADS * HV), 1.0, 6.0, ((0, 8), (1, 4))),
        "lambdas": jnp.clip(jax.random.uniform(keys[3], (HEADS,), jnp.float32, 0.3, 0.8), 0.3, 0.8),
        "query_gain": draw_query_gain(jax.random.fold_in(keys[8], 71), 0),
        "key_gain": draw_key_gain(jax.random.fold_in(keys[8], 71), 0),
        "sub_gain": jnp.clip(1.0 + 0.18 * jax.random.normal(keys[6], (HV,), jnp.float32), 0.1, 1.9),
        "out_weight": bell_draw(keys[7], (HEADS * HV, D), (HEADS * HV) ** -0.5, 0.1875, ((1, 8),)),
    }


epsilon = 1e-06
output_scale = 0.8

def normalize(field, scaling):
    return field * lax.rsqrt(lax.optimization_barrier(jnp.mean(field * field, axis=-1, keepdims=True)) + epsilon) * scaling

def reference(query_rows, key_rows, value_rows, lambdas, query_gain, key_gain, sub_gain, out_weight):
    sequences = query_rows.shape[0]
    length = query_rows.shape[1]
    groups = 2 * HEADS
    query_norm = normalize(query_rows.reshape(sequences, length, groups, HK).astype(jnp.float32), query_gain).astype(jnp.bfloat16)
    key_norm = normalize(key_rows.reshape(sequences, length, groups, HK).astype(jnp.float32), key_gain).astype(jnp.bfloat16)
    value_heads = value_rows.reshape(sequences, length, HEADS, HV)
    value_groups = jnp.concatenate([value_heads, value_heads], axis=2)
    positions = jnp.arange(length)
    causal = positions[None, :] <= positions[:, None]

    def one_group(inputs):
        group_query, group_key, group_value = inputs
        scores = jnp.dot(group_query, group_key.T, preferred_element_type=jnp.float32) * HK ** (-0.5)
        scores = jnp.where(causal, scores, -jnp.inf)
        weights = jax.nn.softmax(scores, axis=-1).astype(jnp.bfloat16)
        return jnp.dot(weights, group_value, preferred_element_type=jnp.float32).astype(jnp.bfloat16)

    def by_group(field):
        return jnp.transpose(field, (0, 2, 1, 3)).reshape(sequences * groups, length, field.shape[3])
    map_outputs = lax.map(one_group, (by_group(query_norm), by_group(key_norm), by_group(value_groups)))
    map_outputs = jnp.transpose(map_outputs.reshape(sequences, groups, length, HV), (0, 2, 1, 3)).astype(jnp.float32)
    mixed_heads = map_outputs[:, :, :HEADS] - lambdas[:, None] * map_outputs[:, :, HEADS:]
    normed = (normalize(mixed_heads, sub_gain) * output_scale).astype(jnp.bfloat16).reshape(sequences * length, HEADS * HV)
    projected = jnp.dot(normed, out_weight, preferred_element_type=jnp.float32)
    return projected.astype(jnp.bfloat16).reshape(sequences, length, D)
```

```python
import functools

import jax
import jax.numpy as jnp
from jax import lax
from jax.experimental import pallas as pl
from jax.experimental.pallas import tpu as pltpu
from jax.sharding import PartitionSpec as P

D = 2048
HEADS = 8
HK = 64
HV = 128


epsilon = 1e-06
output_scale = 0.8


def normalize(field, scaling):
    return field * lax.rsqrt(jnp.mean(field * field, axis=-1, keepdims=True) + epsilon) * scaling


def attend(arrived, length):
    block_rows = max(min(512, length), length // 16)
    results = []
    for number in range(length // block_rows):
        first_row = number * block_rows
        last_row = first_row + block_rows
        query_block = arrived[first_row:last_row, :, :HK]
        key_block = arrived[:last_row, :, HK : 2 * HK]
        value_block = arrived[:last_row, :, 2 * HK :]
        scores = jnp.einsum(
            "qgd,kgd->gqk", query_block, key_block, preferred_element_type=jnp.float32
        ) * HK ** (-0.5)
        visible = jnp.arange(last_row)[None, :] <= (first_row + jnp.arange(block_rows))[:, None]
        scores = jnp.where(visible[None], scores, -jnp.inf)
        weights = jax.nn.softmax(scores, axis=-1).astype(jnp.bfloat16)
        results.append(
            jnp.einsum(
                "gqk,kgd->qgd", weights, value_block, preferred_element_type=jnp.float32
            ).astype(jnp.bfloat16)
        )
    return jnp.concatenate(results, axis=0)


def body(query_rows, key_rows, value_rows, lambdas, query_gain, key_gain, sub_gain, out_weight):
    sequences = query_rows.shape[0]
    tokens_here = query_rows.shape[1]
    groups = 2 * HEADS
    query_norm = normalize(
        query_rows.reshape(sequences, tokens_here, groups, HK).astype(jnp.float32), query_gain
    ).astype(jnp.bfloat16)
    key_norm = normalize(
        key_rows.reshape(sequences, tokens_here, groups, HK).astype(jnp.float32), key_gain
    ).astype(jnp.bfloat16)
    value_heads = value_rows.reshape(sequences, tokens_here, HEADS, HV)
    packet = jnp.concatenate(
        [query_norm, key_norm, jnp.concatenate([value_heads, value_heads], axis=2)], axis=3
    )
    arrived = lax.all_to_all(packet, "sp", split_axis=2, concat_axis=1, tiled=True)
    length = arrived.shape[1]
    map_outputs = attend(arrived[0], length)[None]
    returned = lax.all_to_all(map_outputs, "sp", split_axis=1, concat_axis=2, tiled=True)
    returned_float = returned.astype(jnp.float32)
    mixed_heads = returned_float[:, :, :HEADS] - lambdas[:, None] * returned_float[:, :, HEADS:]
    normed = (
        (normalize(mixed_heads, sub_gain) * output_scale)
        .astype(jnp.bfloat16)
        .reshape(sequences * tokens_here, HEADS * HV)
    )
    projected = jnp.dot(
        normed,
        lax.all_gather(out_weight, "dp", axis=1, tiled=True),
        preferred_element_type=jnp.float32,
    )
    return projected.astype(jnp.bfloat16).reshape(sequences, tokens_here, D)


MESH = pl.DeviceIdType.MESH
TILE = 2 * HK
EVERY = range(HEADS)
LOW, MIDDLE, TOP = (2, 0, 1), (4, 5, 3), (6, 7)
SPLIT = len(LOW) * HV
SEATS = 14


def fits(sp, dp, rows_shape, weight_shape):
    if sp != 4 or dp not in (2, 8) or HEADS != 8 or TILE != 128 or HV != TILE:
        return False
    return rows_shape[0] == 1 and rows_shape[1] % 128 == 0 and rows_shape[1] * sp <= 1024 and weight_shape[1] % 128 == 0


def routes():
    first = {
        0: [("kv", h, 0, 1, h) for h in TOP + MIDDLE + LOW],
        1: [("kv", h, 1, 2, h) for h in MIDDLE] + [("kv", h, 1, 3, h) for h in TOP],
        2: [("all", 2, 2, 1, HEADS), ("all", 6, 2, 3, HEADS), ("all", 7, 2, 3, HEADS + 1),
            ("all", 0, 2, 1, HEADS + 1), ("all", 1, 2, 1, HEADS + 2)],
        3: [("all", h, 3, 2, HEADS + n) for n, h in enumerate(LOW + MIDDLE)],
    }
    passed = {
        1: [("kv", h, 0, 3 if h in TOP else 2, h) for h in TOP + MIDDLE],
        2: [("all", h, 3, 1, HEADS + 3 + n) for n, h in enumerate(LOW)],
    }
    out = {
        1: [("out", h, 2 * n + r - 2, r, 7 if r == 2 else 11) for n, h in enumerate(LOW) for r in (3, 2)],
        2: [("out", h, n, 3, 10) for n, h in enumerate(MIDDLE)],
        3: [("out", h, n, 2, 6) for n, h in enumerate(TOP)],
    }
    return first, passed, out


def kernel(
    sp, dp, q_ref, k_ref, v_ref, lam_in, qg_in, kg_in, sg_in, w_ref, out_ref,
    raw, qkv, ob, nsend, wbuf, acc, lam_ref, qg_ref, kg_ref, sg_ref,
    raw_sem, v_sem, own_sem, small_sem, far_sem, send_sem, in_recv, w_recv, p_recv,
):
    me, d = lax.axis_index("sp"), lax.axis_index("dp")
    swap = 1 - 2 * lax.rem(d, 2)
    partner = d + swap
    chips = dp // 2
    square = chips == 4
    rows = q_ref.shape[0]
    depth, columns = w_ref.shape
    half = depth // 2
    first, passed, out = routes()

    def fellow(c):
        core, chip = lax.rem(d, 2), d // 2
        x, y = lax.rem(chip, 2), chip // 2
        x = 1 - x if c % 2 else x
        y = 1 - y if c // 2 else y
        return (y * 2 + x) * 2 + core

    def role(body):
        for z in range(sp):
            @pl.when(me == z)
            def _(z=z):
                body(z)

    barrier = pltpu.get_barrier_semaphore()

    def greet(z, device):
        pl.semaphore_signal(barrier, inc=1, device_id=(z, device), device_id_type=MESH)

    beside = (1, 2) if square else ()
    greet(me, partner)
    for c in beside:
        greet(me, fellow(c))

    def neighbours(z):
        return [n for n in (z - 1, z + 1) if 0 <= n < sp]

    def greet_line(z):
        for n in neighbours(z):
            greet(n, d)

    role(greet_line)

    small = [
        pltpu.make_async_copy(src, dst, small_sem.at[n])
        for n, (src, dst) in enumerate(((lam_in, lam_ref), (qg_in, qg_ref), (kg_in, kg_ref), (sg_in, sg_ref)))
    ]

    def rows_of(h):
        return pl.ds(h * half, half)

    def own_weights():
        return pltpu.make_async_copy(w_ref, wbuf.at[d], own_sem)

    for n, src in enumerate((k_ref, q_ref)):
        pltpu.make_async_copy(src, raw.at[n], raw_sem.at[n]).start()
    for copy in small:
        copy.start()
    own_weights().start()
    for h in EVERY:
        pltpu.make_async_copy(v_ref.at[:, pl.ds(h * HV, HV)], qkv.at[h, me, 1], v_sem).start()

    def remote(src, dst, recv, to):
        return pltpu.make_async_remote_copy(
            src_ref=src, dst_ref=dst, send_sem=send_sem, recv_sem=recv, device_id=to, device_id_type=MESH,
        )

    def spread(c, h):
        source, over = d, c
        if c == 3:
            source, over = fellow(1 + h), 2 - h
        piece = wbuf.at[source, rows_of(h)]
        return remote(piece, piece, w_recv.at[2 * c - 2 + h], (me, fellow(over)))

    def gained(c, h):
        piece = wbuf.at[fellow(c), rows_of(h)]
        remote(piece, piece, w_recv.at[2 * c - 2 + h], (me, partner)).wait_recv()

    def pair(c, h=None, at=None):
        at = fellow(c) if at is None else at
        piece = wbuf.at[at] if h is None else wbuf.at[at, rows_of(h)]
        return remote(piece, piece, p_recv.at[c + (h or 0)], (me, partner))

    def paired(c, h=None):
        pair(c, h, fellow(c) + swap).wait_recv()

    def put(key):
        kind, h, r, to, n = key
        if kind == "out":
            return remote(nsend.at[r], ob.at[:, pl.ds(h * HV, HV)], in_recv.at[n], (to, d))
        piece = qkv.at[h, r, pl.ds(0, 2)] if kind == "kv" else qkv.at[h, r]
        return remote(piece, piece, in_recv.at[n], (to, d))

    def got(piece, n):
        remote(piece, piece, in_recv.at[n], (me, partner)).wait_recv()

    def got_kv(h, count=1):
        got(qkv.at[h, 0, pl.ds(0, 2)] if count == 1 else qkv.at[h, pl.ds(0, 2), pl.ds(0, 2)], h)

    def got_all(h, r, n):
        got(qkv.at[h, r], HEADS + n)

    def weights_start():
        own_weights().wait()
        for order in range(2):
            for c in beside:
                spread(c, (c + 1 + order) % 2).start()
        pair(0).start()

    def weights_first():
        if square:
            for h in range(2):
                gained(1 + h, h)
                spread(3, h).start()

    def weights_next():
        if square:
            for h in range(2):
                gained(1 + h, 1 - h)
                pair(1 + h).start()

    def weights_last():
        if square:
            for h in range(2):
                gained(3, h)
                pair(3, h).start()

    pl.semaphore_wait(barrier, 1 + len(beside) + 2 - jnp.where((me == 0) | (me == sp - 1), 1, 0))

    @pl.when(me == 2)
    def _():
        pl.semaphore_signal(far_sem, inc=1, device_id=(1, d), device_id_type=MESH)

    weights_start()
    for copy in small:
        copy.wait()

    lane = lax.broadcasted_iota(jnp.int32, (2 * TILE, TILE), 1) // HK
    from_lane = lax.rem(lax.broadcasted_iota(jnp.int32, (2 * TILE, TILE), 0), TILE) // HK
    ones = (lane == from_lane).astype(jnp.bfloat16)
    early = lax.broadcasted_iota(jnp.int32, (rows, TILE), 1) < HK
    visible = lax.broadcasted_iota(jnp.int32, (rows, rows), 1) <= lax.broadcasted_iota(jnp.int32, (rows, rows), 0)
    visible = jnp.concatenate([visible] * 2, axis=0)
    gains = [jnp.concatenate([ref[...]] * 2, axis=1) for ref in (kg_ref, qg_ref)]
    sub_gain = sg_ref[...] * output_scale
    decay = HK ** (-0.5) * 1.4426950408889634

    def normed_rows(block, gain):
        field = block.astype(jnp.float32)
        square = field * field
        upper = square.astype(jnp.bfloat16)
        lower = (square - upper.astype(jnp.float32)).astype(jnp.bfloat16)
        total = jnp.dot(jnp.concatenate([upper, lower], axis=1), ones, preferred_element_type=jnp.float32)
        return field * lax.rsqrt(total * (1.0 / HK) + epsilon) * gain

    def own_rows(z, n, p):
        here = [
            normed_rows(raw[n, :, m * HEADS * HK + p * TILE : m * HEADS * HK + (p + 1) * TILE], gains[n])
            for m in range(2)
        ]
        there = [pltpu.roll(x, HK, axis=1) for x in here]
        qkv[2 * p, z, 2 * n] = jnp.where(early, here[0], there[1]).astype(jnp.bfloat16)
        qkv[2 * p + 1, z, 2 * n] = jnp.where(early, there[0], here[1]).astype(jnp.bfloat16)

    def unit(h, r):
        query = qkv[h, r, 2]
        zero = jnp.zeros_like(query)
        stacked = jnp.concatenate([jnp.where(early, query, zero), jnp.where(early, zero, query)], axis=0)
        keys = qkv[h, : r + 1, 0].reshape((r + 1) * rows, TILE)
        values = qkv[h, : r + 1, 1].reshape((r + 1) * rows, HV)
        scores = lax.dot_general(stacked, keys, (((1,), (1,)), ((), ())), preferred_element_type=jnp.float32)
        last = jnp.where(visible, scores[:, r * rows :], -jnp.inf)
        scores = last if r == 0 else jnp.concatenate([scores[:, : r * rows], last], axis=1)
        raised = jnp.exp2((scores - jnp.max(scores, axis=1, keepdims=True)) * decay)
        weights = (raised * (1.0 / jnp.sum(raised, axis=1, keepdims=True))).astype(jnp.bfloat16)
        maps = jnp.dot(weights, values, preferred_element_type=jnp.float32).astype(jnp.bfloat16).astype(jnp.float32)
        mixed = maps[:rows] - lam_ref[h] * maps[rows:]
        mean = jnp.mean(mixed * mixed, axis=1, keepdims=True)
        return (mixed * lax.rsqrt(mean + epsilon) * sub_gain).astype(jnp.bfloat16)

    def keep(h, r):
        ob[:, h * HV : (h + 1) * HV] = unit(h, r)

    def give(z, key):
        kind, h, slot, to, n = key
        nsend[slot] = unit(h, to)

    def start(keys):
        for key in keys:
            put(key).start()

    def rows_ready(n):
        pltpu.make_async_copy(raw.at[n], raw.at[n], raw_sem.at[n]).wait()

    def values_ready():
        pltpu.make_async_copy(qkv.at[:, me, 1], qkv.at[:, me, 1], v_sem).wait()

    def prepare(z, order):
        waiting = list(first[z])
        with_query = z > 1
        done = set()

        def flush():
            while waiting and waiting[0][1] in done:
                put(waiting.pop(0)).start()

        rows_ready(0)
        if with_query:
            rows_ready(1)
        for count, p in enumerate(order):
            own_rows(z, 0, p)
            if with_query:
                own_rows(z, 1, p)
            if count == 0:
                values_ready()
            if z == 1 and 2 * p in TOP:
                pl.semaphore_wait(far_sem, 1)
            done.update((2 * p, 2 * p + 1))
            flush()
        if not with_query:
            rows_ready(1)
            for p in order:
                own_rows(z, 1, p)

    def part(z):
        if z == 0:
            prepare(z, (3, 2, 1, 0))
            for h in EVERY:
                keep(h, 0)
            weights_first()
            weights_next()
        if z == 1:
            prepare(z, (2, 1, 3, 0))
            for n, key in enumerate(passed[1]):
                got_kv(key[1])
                put(key).start()
                keep(key[1], 1)
                if n == 2:
                    weights_first()
            for n, h in enumerate(LOW):
                got_kv(h)
                got_all(h, 2, n)
                got_all(h, 3, 3 + n)
                for key in out[1][2 * n : 2 * n + 2]:
                    give(z, key)
                keep(h, 1)
                start(out[1][2 * n : 2 * n + 2])
                if n == 1:
                    weights_next()
        if z == 2:
            prepare(z, (1, 3, 0, 2))
            for n, key in enumerate(passed[2]):
                got_all(key[1], 3, n)
                put(key).start()
            weights_first()
            for n, h in enumerate(MIDDLE):
                got_kv(h, 2)
                got_all(h, 3, 3 + n)
                give(z, out[2][n])
                keep(h, 2)
                put(out[2][n]).start()
                if n == 0:
                    weights_next()
        if z == 3:
            prepare(z, (1, 0, 2, 3))
            weights_first()
            for n, h in enumerate(TOP):
                got_kv(h, 2)
                got_all(h, 2, n)
                give(z, out[3][n])
                keep(h, 3)
                put(out[3][n]).start()
            weights_next()

    role(part)

    def project(shard, lower):
        where = slice(0, SPLIT) if lower else slice(SPLIT, depth)
        here = pl.ds(pl.multiple_of(shard * columns, 128), columns)
        total = jnp.dot(ob[:, where], wbuf[shard, where, :], preferred_element_type=jnp.float32)
        if lower:
            out_ref[:, here] = (acc[:, here] + total).astype(jnp.bfloat16)
        else:
            acc[:, here] = total

    def outputs(which):
        def body(z):
            if z == 2:
                if which:
                    got(ob.at[:, pl.ds(0, len(TOP) * HV)], 6)
                else:
                    got(ob.at[:, pl.ds(0, SPLIT)], 7)
            if z == 3:
                if which:
                    got(ob.at[:, pl.ds(0, len(MIDDLE) * HV)], 10)
                else:
                    got(ob.at[:, pl.ds(0, SPLIT)], 11)
        role(body)

    weights_last()
    outputs(True)
    paired(0)
    for c in beside:
        paired(c)
    for c in range(chips):
        project(fellow(c), False)
        if c < 3:
            project(fellow(c) + swap, False)
    if square:
        for h in range(2):
            paired(3, h)
        project(fellow(3) + swap, False)
    outputs(False)
    for c in range(chips):
        project(fellow(c), True)
        project(fellow(c) + swap, True)

    def drain(z):
        for keys in (first, passed, out):
            for key in keys.get(z, ()):
                put(key).wait_send()

    role(drain)
    pair(0).wait_send()
    if square:
        for c in range(1, chips):
            for h in range(2):
                spread(c, h).wait_send()
            pair(c).wait_send()


def fused(sp, dp, query_rows, key_rows, value_rows, lambdas, query_gain, key_gain, sub_gain, out_weight):
    rows = query_rows.shape[1]
    depth, columns = out_weight.shape
    vmem = pl.BlockSpec(memory_space=pltpu.VMEM)
    hbm = pl.BlockSpec(memory_space=pl.ANY)
    dma = pltpu.SemaphoreType.DMA
    out = pl.pallas_call(
        functools.partial(kernel, sp, dp),
        out_shape=pltpu.VMEM((rows, columns * dp), jnp.bfloat16),
        in_specs=[hbm] * 8,
        out_specs=vmem,
        scratch_shapes=[
            pltpu.VMEM((2, rows, 2 * HEADS * HK), jnp.bfloat16),
            pltpu.VMEM((HEADS, sp, 3, rows, TILE), jnp.bfloat16),
            pltpu.VMEM((rows, HEADS * HV), jnp.bfloat16),
            pltpu.VMEM((2 * len(LOW), rows, HV), jnp.bfloat16),
            pltpu.VMEM((dp, depth, columns), jnp.bfloat16),
            pltpu.VMEM((rows, columns * dp), jnp.float32),
            pltpu.SMEM(lambdas.shape, jnp.float32),
            pltpu.VMEM((1, HK), jnp.float32), pltpu.VMEM((1, HK), jnp.float32), pltpu.VMEM((1, HV), jnp.float32),
            dma((2,)), dma, dma, dma((4,)), pltpu.SemaphoreType.REGULAR, dma, dma((SEATS,)), dma((6,)), dma((5,)),
        ],
        compiler_params=pltpu.CompilerParams(collective_id=0, has_side_effects=True),
    )(
        query_rows[0], key_rows[0], value_rows[0], lambdas,
        query_gain[None], key_gain[None], sub_gain[None], out_weight,
    )
    return out[None]


def solution(mesh):
    in_specs = (
        P("dp", "sp", None),
        P("dp", "sp", None),
        P("dp", "sp", None),
        P(),
        P(),
        P(),
        P(),
        P(None, "dp"),
    )
    out_specs = P("dp", "sp", None)
    sp, dp = mesh.shape["sp"], mesh.shape["dp"]

    def step(*operands):
        if fits(sp, dp, operands[0].shape, operands[7].shape):
            return fused(sp, dp, *operands)
        return body(*operands)

    return jax.shard_map(step, mesh=mesh, in_specs=in_specs, out_specs=out_specs, check_vma=False)
```

```python
import functools

import jax
import jax.numpy as jnp
from jax import lax
from jax.experimental import pallas as pl
from jax.experimental.pallas import tpu as pltpu
from jax.sharding import PartitionSpec as P

D = 2048
HEADS = 8
HK = 64
HV = 128


epsilon = 1e-06
output_scale = 0.8


def normalize(field, scaling):
    return field * lax.rsqrt(jnp.mean(field * field, axis=-1, keepdims=True) + epsilon) * scaling


def attend(arrived, length):
    block_rows = max(min(512, length), length // 16)
    results = []
    for number in range(length // block_rows):
        first_row = number * block_rows
        last_row = first_row + block_rows
        query_block = arrived[first_row:last_row, :, :HK]
        key_block = arrived[:last_row, :, HK : 2 * HK]
        value_block = arrived[:last_row, :, 2 * HK :]
        scores = jnp.einsum(
            "qgd,kgd->gqk", query_block, key_block, preferred_element_type=jnp.float32
        ) * HK ** (-0.5)
        visible = jnp.arange(last_row)[None, :] <= (first_row + jnp.arange(block_rows))[:, None]
        scores = jnp.where(visible[None], scores, -jnp.inf)
        weights = jax.nn.softmax(scores, axis=-1).astype(jnp.bfloat16)
        results.append(
            jnp.einsum(
                "gqk,kgd->qgd", weights, value_block, preferred_element_type=jnp.float32
            ).astype(jnp.bfloat16)
        )
    return jnp.concatenate(results, axis=0)


def body(query_rows, key_rows, value_rows, lambdas, query_gain, key_gain, sub_gain, out_weight):
    sequences = query_rows.shape[0]
    tokens_here = query_rows.shape[1]
    groups = 2 * HEADS
    query_norm = normalize(
        query_rows.reshape(sequences, tokens_here, groups, HK).astype(jnp.float32), query_gain
    ).astype(jnp.bfloat16)
    key_norm = normalize(
        key_rows.reshape(sequences, tokens_here, groups, HK).astype(jnp.float32), key_gain
    ).astype(jnp.bfloat16)
    value_heads = value_rows.reshape(sequences, tokens_here, HEADS, HV)
    packet = jnp.concatenate(
        [query_norm, key_norm, jnp.concatenate([value_heads, value_heads], axis=2)], axis=3
    )
    arrived = lax.all_to_all(packet, "sp", split_axis=2, concat_axis=1, tiled=True)
    length = arrived.shape[1]
    map_outputs = attend(arrived[0], length)[None]
    returned = lax.all_to_all(map_outputs, "sp", split_axis=1, concat_axis=2, tiled=True)
    returned_float = returned.astype(jnp.float32)
    mixed_heads = returned_float[:, :, :HEADS] - lambdas[:, None] * returned_float[:, :, HEADS:]
    normed = (
        (normalize(mixed_heads, sub_gain) * output_scale)
        .astype(jnp.bfloat16)
        .reshape(sequences * tokens_here, HEADS * HV)
    )
    projected = jnp.dot(
        normed,
        lax.all_gather(out_weight, "dp", axis=1, tiled=True),
        preferred_element_type=jnp.float32,
    )
    return projected.astype(jnp.bfloat16).reshape(sequences, tokens_here, D)


MESH = pl.DeviceIdType.MESH
TILE = 2 * HK
EVERY = range(HEADS)
LOW, MIDDLE, TOP = (0, 1, 2), (4, 5, 3), (6, 7)
SEATS = 14


def fits(sp, dp, rows_shape, weight_shape):
    if sp != 4 or dp not in (2, 8) or HEADS != 8 or TILE != 128 or HV != TILE:
        return False
    return rows_shape[0] == 1 and rows_shape[1] % 128 == 0 and rows_shape[1] * sp <= 1024 and weight_shape[1] % 128 == 0


def routes():
    first = {
        0: [("kv", h, 0, 1, h) for h in (6, 7, 0, 4, 5, 1, 3, 2)],
        1: [("kv", h, 1, 2, h) for h in MIDDLE] + [("kv", h, 1, 3, h) for h in TOP],
        2: [("all", 0, 2, 1, HEADS), ("all", 1, 2, 1, HEADS + 1), ("all", 6, 2, 3, HEADS), ("all", 7, 2, 3, HEADS + 1),
            ("all", 2, 2, 1, HEADS + 2)],
        3: [("all", h, 3, 2, HEADS + n) for n, h in enumerate(LOW + MIDDLE)],
    }
    passed = {
        1: [("kv", h, 0, 3 if h in TOP else 2, h) for h in TOP + MIDDLE],
        2: [("all", h, 3, 1, HEADS + 3 + n) for n, h in enumerate(LOW)],
    }
    out = {
        1: [("out", h, n, 2, 6 if n < 2 else 7) for n, h in enumerate(LOW)]
        + [("out", h, 3 + n, 3, 10 if n < 2 else 11) for n, h in enumerate(LOW)],
        2: [("out", h, n, 3, 12 if n < 2 else 13) for n, h in enumerate(MIDDLE)],
        3: [("out", h, n, 2, 1) for n, h in enumerate(TOP)],
    }
    return first, passed, out


def kernel(
    sp, dp, q_ref, k_ref, v_ref, lam_in, qg_in, kg_in, sg_in, w_ref, out_ref,
    raw, qkv, ob, nsend, wbuf, acc, lam_ref, qg_ref, kg_ref, sg_ref,
    raw_sem, v_sem, own_sem, small_sem, far_sem, send_sem, in_recv, w_recv, p_recv,
):
    me, d = lax.axis_index("sp"), lax.axis_index("dp")
    swap = 1 - 2 * lax.rem(d, 2)
    partner = d + swap
    chips = dp // 2
    square = chips == 4
    rows = q_ref.shape[0]
    depth, columns = w_ref.shape
    half = depth // 2
    first, passed, out = routes()

    def fellow(c):
        core, chip = lax.rem(d, 2), d // 2
        x, y = lax.rem(chip, 2), chip // 2
        x = 1 - x if c % 2 else x
        y = 1 - y if c // 2 else y
        return (y * 2 + x) * 2 + core

    def role(body):
        for z in range(sp):
            @pl.when(me == z)
            def _(z=z):
                body(z)

    barrier = pltpu.get_barrier_semaphore()

    def greet(z, device):
        pl.semaphore_signal(barrier, inc=1, device_id=(z, device), device_id_type=MESH)

    beside = (1, 2) if square else ()
    greet(me, partner)
    for c in beside:
        greet(me, fellow(c))

    def neighbours(z):
        return [n for n in (z - 1, z + 1) if 0 <= n < sp]

    def greet_line(z):
        for n in neighbours(z):
            greet(n, d)

    role(greet_line)

    small = [
        pltpu.make_async_copy(src, dst, small_sem.at[n])
        for n, (src, dst) in enumerate(((lam_in, lam_ref), (qg_in, qg_ref), (kg_in, kg_ref), (sg_in, sg_ref)))
    ]

    def rows_of(h):
        return pl.ds(h * half, half)

    def own_weights():
        return pltpu.make_async_copy(w_ref, wbuf.at[d], own_sem)

    for n, src in enumerate((k_ref, q_ref)):
        pltpu.make_async_copy(src, raw.at[n], raw_sem.at[n]).start()
    for copy in small:
        copy.start()
    own_weights().start()
    for h in EVERY:
        pltpu.make_async_copy(v_ref.at[:, pl.ds(h * HV, HV)], qkv.at[h, me, 1], v_sem).start()

    def remote(src, dst, recv, to):
        return pltpu.make_async_remote_copy(
            src_ref=src, dst_ref=dst, send_sem=send_sem, recv_sem=recv, device_id=to, device_id_type=MESH,
        )

    def piece(device, h, j=None):
        size = half if j is None else half // 2
        return wbuf.at[device, pl.ds(h * half + (j or 0) * size, size)]

    def seat(c, h, j=None):
        return 2 * c - 2 + h if j is None else 4 + 2 * h + j

    def spread(c, h, j=None):
        source, over = d, c
        if c == 3:
            source, over = fellow(1 + h), 2 - h
        block = piece(source, h, j)
        return remote(block, block, w_recv.at[seat(c, h, j)], (me, fellow(over)))

    def gained(c, h, j=None):
        block = piece(fellow(c), h, j)
        remote(block, block, w_recv.at[seat(c, h, j)], (me, partner)).wait_recv()

    def pair(c, h=None, j=None, at=None):
        at = fellow(c) if at is None else at
        block = wbuf.at[at] if h is None else piece(at, h, j)
        return remote(block, block, p_recv.at[c + (2 * h + j if h is not None else 0)], (me, partner))

    def paired(c, h=None, j=None):
        pair(c, h, j, fellow(c) + swap).wait_recv()

    def put(key):
        kind, h, r, to, n = key
        if kind == "out":
            return remote(nsend.at[r], ob.at[:, pl.ds(h * HV, HV)], in_recv.at[n], (to, d))
        piece = qkv.at[h, r, pl.ds(0, 2)] if kind == "kv" else qkv.at[h, r]
        return remote(piece, piece, in_recv.at[n], (to, d))

    def got(piece, n):
        remote(piece, piece, in_recv.at[n], (me, partner)).wait_recv()

    def got_kv(h, count=1):
        got(qkv.at[h, 0, pl.ds(0, 2)] if count == 1 else qkv.at[h, pl.ds(0, 2), pl.ds(0, 2)], h)

    def got_all(h, r, n):
        got(qkv.at[h, r], HEADS + n)

    def weights_start():
        own_weights().wait()
        for order in range(2):
            for c in beside:
                spread(c, (c + 1 + order) % 2).start()
        pair(0).start()

    def weights_first():
        if square:
            for h in range(2):
                gained(1 + h, h)
                for j in range(2):
                    spread(3, h, j).start()

    def weights_next():
        if square:
            for h in range(2):
                gained(1 + h, 1 - h)
                pair(1 + h).start()

    def weights_last():
        if square:
            for j in range(2):
                for h in range(2):
                    gained(3, h, j)
                    pair(3, h, j).start()

    for copy in small:
        copy.wait()

    lane = lax.broadcasted_iota(jnp.int32, (2 * TILE, TILE), 1) // HK
    from_lane = lax.rem(lax.broadcasted_iota(jnp.int32, (2 * TILE, TILE), 0), TILE) // HK
    ones = (lane == from_lane).astype(jnp.bfloat16)
    early = lax.broadcasted_iota(jnp.int32, (rows, TILE), 1) < HK
    visible = lax.broadcasted_iota(jnp.int32, (rows, rows), 1) <= lax.broadcasted_iota(jnp.int32, (rows, rows), 0)
    visible = jnp.concatenate([visible] * 2, axis=0)
    gains = [jnp.concatenate([ref[...]] * 2, axis=1) for ref in (kg_ref, qg_ref)]
    sub_gain = sg_ref[...] * output_scale
    decay = HK ** (-0.5) * 1.4426950408889634

    def normed_rows(block, gain):
        field = block.astype(jnp.float32)
        square = field * field
        upper = square.astype(jnp.bfloat16)
        lower = (square - upper.astype(jnp.float32)).astype(jnp.bfloat16)
        total = jnp.dot(jnp.concatenate([upper, lower], axis=1), ones, preferred_element_type=jnp.float32)
        return field * lax.rsqrt(total * (1.0 / HK) + epsilon) * gain

    def own_rows(z, n, p):
        here = [
            normed_rows(raw[n, :, m * HEADS * HK + p * TILE : m * HEADS * HK + (p + 1) * TILE], gains[n])
            for m in range(2)
        ]
        there = [pltpu.roll(x, HK, axis=1) for x in here]
        qkv[2 * p, z, 2 * n] = jnp.where(early, here[0], there[1]).astype(jnp.bfloat16)
        qkv[2 * p + 1, z, 2 * n] = jnp.where(early, there[0], here[1]).astype(jnp.bfloat16)

    def unit(h, r):
        query = qkv[h, r, 2]
        zero = jnp.zeros_like(query)
        stacked = jnp.concatenate([jnp.where(early, query, zero), jnp.where(early, zero, query)], axis=0)
        keys = qkv[h, : r + 1, 0].reshape((r + 1) * rows, TILE)
        values = qkv[h, : r + 1, 1].reshape((r + 1) * rows, HV)
        scores = lax.dot_general(stacked, keys, (((1,), (1,)), ((), ())), preferred_element_type=jnp.float32)
        last = jnp.where(visible, scores[:, r * rows :], -jnp.inf)
        scores = last if r == 0 else jnp.concatenate([scores[:, : r * rows], last], axis=1)
        raised = jnp.exp2((scores - jnp.max(scores, axis=1, keepdims=True)) * decay)
        weights = (raised * (1.0 / jnp.sum(raised, axis=1, keepdims=True))).astype(jnp.bfloat16)
        maps = jnp.dot(weights, values, preferred_element_type=jnp.float32).astype(jnp.bfloat16).astype(jnp.float32)
        mixed = maps[:rows] - lam_ref[h] * maps[rows:]
        mean = jnp.mean(mixed * mixed, axis=1, keepdims=True)
        return (mixed * lax.rsqrt(mean + epsilon) * sub_gain).astype(jnp.bfloat16)

    def keep(h, r):
        ob[:, h * HV : (h + 1) * HV] = unit(h, r)

    def give(z, key):
        kind, h, slot, to, n = key
        nsend[slot] = unit(h, to)

    def start(keys):
        for key in keys:
            put(key).start()

    def rows_ready(n):
        pltpu.make_async_copy(raw.at[n], raw.at[n], raw_sem.at[n]).wait()

    def values_ready():
        pltpu.make_async_copy(qkv.at[:, me, 1], qkv.at[:, me, 1], v_sem).wait()

    orders = {0: (3, 0, 2, 1), 1: (2, 1, 3, 0), 2: (0, 3, 1, 2), 3: (0, 1, 2, 3)}

    def before(z):
        rows_ready(0)
        if z > 1:
            rows_ready(1)
        for n in range(2 if z > 1 else 1):
            own_rows(z, n, orders[z][0])

    role(before)
    pl.semaphore_wait(barrier, 1 + len(beside) + 2 - jnp.where((me == 0) | (me == sp - 1), 1, 0))

    @pl.when(me == 2)
    def _():
        pl.semaphore_signal(far_sem, inc=1, device_id=(1, d), device_id_type=MESH)

    weights_start()
    values_ready()

    def prepare(z):
        waiting = list(first[z])
        done = set()
        for count, p in enumerate(orders[z]):
            if count:
                for n in range(2 if z > 1 else 1):
                    own_rows(z, n, p)
            if z == 1 and 2 * p in TOP:
                pl.semaphore_wait(far_sem, 1)
            done.update((2 * p, 2 * p + 1))
            while waiting and waiting[0][1] in done:
                put(waiting.pop(0)).start()
        if z < 2:
            rows_ready(1)
            for p in orders[z]:
                own_rows(z, 1, p)

    def project(shards, pieces, store):
        for shard in shards:
            here = pl.ds(pl.multiple_of(shard * columns, 128), columns)
            total = None if "new" in store else acc[:, here]
            for a, b in pieces:
                where = slice(a * HV, b * HV)
                part = jnp.dot(ob[:, where], wbuf[shard, where, :], preferred_element_type=jnp.float32)
                total = part if total is None else total + part
            if "end" in store:
                out_ref[:, here] = total.astype(jnp.bfloat16)
            else:
                acc[:, here] = total

    own = [fellow(c) for c in range(min(chips, 3))]
    theirs = [fellow(c) + swap for c in range(min(chips, 3))]
    last_own = [fellow(3)] if square else []
    last_theirs = [fellow(3) + swap] if square else []

    def weights_mid():
        paired(0)
        for c in beside:
            paired(c)

    def weights_end():
        if square:
            for j in range(2):
                for h in range(2):
                    paired(3, h, j)

    whole = ((0, HEADS),)

    def part_0():
        for h in EVERY:
            keep(h, 0)
        paired(0)
        project([own[0], theirs[0]], whole, "new end")
        weights_first()
        weights_next()
        project(own[1:], whole, "new end")
        for c in beside:
            paired(c)
        project(theirs[1:], whole, "new end")
        weights_last()
        project(last_own, whole, "new end")
        weights_end()
        project(last_theirs, whole, "new end")

    def relay(n):
        got_kv(passed[1][n][1])
        put(passed[1][n]).start()
        keep(passed[1][n][1], 1)

    def lower_two(n):
        got_kv(LOW[n])
        got_all(LOW[n], 2, n)
        keep(LOW[n], 1)
        give(1, out[1][n])

    def lower_three(n):
        got_all(LOW[n], 3, 3 + n)
        give(1, out[1][3 + n])
        put(out[1][3 + n]).start()

    def part_1():
        relay(0)
        relay(1)
        lower_two(0)
        relay(2)
        weights_first()
        relay(3)
        lower_two(1)
        relay(4)
        start(out[1][:2])
        lower_three(0)
        lower_two(2)
        lower_three(1)
        put(out[1][2]).start()
        weights_next()
        lower_three(2)
        weights_mid()
        project(own + theirs, whole, "new end")
        weights_last()
        project(last_own, whole, "new end")
        weights_end()
        project(last_theirs, whole, "new end")

    def part_2():
        for n, key in enumerate(passed[2]):
            got_all(key[1], 3, n)
            put(key).start()
        weights_first()
        for n, h in enumerate(MIDDLE):
            got_kv(h, 2)
            got_all(h, 3, 3 + n)
            give(2, out[2][n])
            put(out[2][n]).start()
            keep(h, 2)
            if n == 0:
                weights_next()
        weights_mid()
        got(ob.at[:, pl.ds(0, 2 * HV)], 1)
        project(own + theirs, ((4, 8),), "new")
        weights_last()
        got(ob.at[:, pl.ds(0, 2 * HV)], 6)
        project(own + theirs, ((0, 2),), "")
        project(last_own, ((0, 2), (4, 8)), "new")
        weights_end()
        project(last_theirs, ((0, 2), (4, 8)), "new")
        got(ob.at[:, pl.ds(0, HV)], 7)
        project(own + theirs + last_own + last_theirs, ((2, 4),), "end")

    def part_3():
        weights_first()
        for n, h in enumerate(TOP):
            got_kv(h, 2)
            got_all(h, 2, n)
            give(3, out[3][n])
            put(out[3][n]).start()
            keep(h, 3)
        weights_next()
        weights_mid()
        project(own + theirs, ((6, 8),), "new")
        weights_last()
        got(ob.at[:, pl.ds(0, 2 * HV)], 12)
        got(ob.at[:, pl.ds(0, 2 * HV)], 10)
        project(own + theirs, ((0, 2), (4, 6)), "")
        project(last_own, ((0, 2), (4, 8)), "new")
        weights_end()
        project(last_theirs, ((0, 2), (4, 8)), "new")
        got(ob.at[:, pl.ds(0, HV)], 13)
        got(ob.at[:, pl.ds(0, HV)], 11)
        project(own + theirs + last_own + last_theirs, ((2, 4),), "end")

    def part(z):
        prepare(z)
        (part_0, part_1, part_2, part_3)[z]()
        for keys in (first, passed, out):
            for key in keys.get(z, ()):
                put(key).wait_send()

    role(part)
    pair(0).wait_send()
    if square:
        for c in range(1, chips):
            for h in range(2):
                spread(c, h).wait_send()
            pair(c).wait_send()


def fused(sp, dp, query_rows, key_rows, value_rows, lambdas, query_gain, key_gain, sub_gain, out_weight):
    rows = query_rows.shape[1]
    depth, columns = out_weight.shape
    vmem = pl.BlockSpec(memory_space=pltpu.VMEM)
    hbm = pl.BlockSpec(memory_space=pl.ANY)
    dma = pltpu.SemaphoreType.DMA
    out = pl.pallas_call(
        functools.partial(kernel, sp, dp),
        out_shape=pltpu.VMEM((rows, columns * dp), jnp.bfloat16),
        in_specs=[hbm] * 8,
        out_specs=vmem,
        scratch_shapes=[
            pltpu.VMEM((2, rows, 2 * HEADS * HK), jnp.bfloat16),
            pltpu.VMEM((HEADS, sp, 3, rows, TILE), jnp.bfloat16),
            pltpu.VMEM((rows, HEADS * HV), jnp.bfloat16),
            pltpu.VMEM((2 * len(LOW), rows, HV), jnp.bfloat16),
            pltpu.VMEM((dp, depth, columns), jnp.bfloat16),
            pltpu.VMEM((rows, columns * dp), jnp.float32),
            pltpu.SMEM(lambdas.shape, jnp.float32),
            pltpu.VMEM((1, HK), jnp.float32), pltpu.VMEM((1, HK), jnp.float32), pltpu.VMEM((1, HV), jnp.float32),
            dma((2,)), dma, dma, dma((4,)), pltpu.SemaphoreType.REGULAR, dma, dma((SEATS,)), dma((8,)), dma((7,)),
        ],
        compiler_params=pltpu.CompilerParams(collective_id=0, has_side_effects=True),
    )(
        query_rows[0], key_rows[0], value_rows[0], lambdas,
        query_gain[None], key_gain[None], sub_gain[None], out_weight,
    )
    return out[None]


def solution(mesh):
    in_specs = (
        P("dp", "sp", None),
        P("dp", "sp", None),
        P("dp", "sp", None),
        P(),
        P(),
        P(),
        P(),
        P(None, "dp"),
    )
    out_specs = P("dp", "sp", None)
    sp, dp = mesh.shape["sp"], mesh.shape["dp"]

    def step(*operands):
        if fits(sp, dp, operands[0].shape, operands[7].shape):
            return fused(sp, dp, *operands)
        return body(*operands)

    return jax.shard_map(step, mesh=mesh, in_specs=in_specs, out_specs=out_specs, check_vma=False)
```
